32 devices in a mesh: sp: 16 (over z, y, x), tp: 2 (over core).
Axes of the slice: x: 2, y: 2, z: 4, core: 2. Of those that a mesh axis runs over, the one named last changes fastest.
Arguments:
- stream_in: bfloat16 [2048, 2048], P(('sp', 'tp')), may hold values from -6 to 6
- query_rows: bfloat16 [2048, 2048], P('sp', 'tp'), may hold values from -6 to 6
- key_rows: bfloat16 [2048, 2048], P('sp', 'tp'), may hold values from -6 to 6
- value_rows: bfloat16 [2048, 2048], P('sp', 'tp'), may hold values from -6 to 6
- removal_key: bfloat16 [2048, 2048], P('sp', 'tp'), may hold values from -6 to 6
- learn_pre: bfloat16 [2048, 2048], P('sp', 'tp'), may hold values from -12 to 4
- log_rate: float32 [2048, 2048], P('sp', 'tp'), may hold values from -14 to 0
- norm_gain: bfloat16 [2048], P('tp'), may hold values from 0.099609375 to 1.8984375
- out_weight: bfloat16 [2048, 2048], replicated, may hold values from -0.125 to 0.125
- ffn_gain: bfloat16 [2048], replicated, may hold values from 0.099609375 to 1.8984375
- routes: int32 [2048, 2], P(('sp', 'tp')), may hold values from 0 to 7, all different within a row; in each aligned block of 64 rows (0 to 63, 64 to 127, ...) at most 32 rows name the same one
- route_weight: float32 [2048, 2], P(('sp', 'tp')), may hold values from 0.1 to 1
- expert_gate: bfloat16 [16, 2048, 1792], P('sp', None, 'tp'), may hold values from -0.125 to 0.125
- expert_up: bfloat16 [16, 2048, 1792], P('sp', None, 'tp'), may hold values from -0.125 to 0.125
- expert_down: bfloat16 [16, 1792, 2048], P('sp', 'tp'), may hold values from -0.09375 to 0.09375
Outputs:
- layer_out: bfloat16 [2048, 2048], P(('sp', 'tp'))
The draws below stay inside these ranges and needn't reach their ends.
Inputs may be any that keep to these rules, and one draw needn't show every extreme that they name: `routes`: in each aligned block of 64 rows (the rows of one device after the mixer) no expert is named by more than 32 rows, a bound that some expert reaches in some or all blocks; the experts of one row differ.
All inputs are finite; a program needn't handle non-finite values.
Results may differ from the reference program's by a relative error of at most 0.0065.
Values may be sent and summed in bfloat16 or wider, within the bound.
A program may use at most 192 MiB of HBM per device.

```python
import math
import jax
import jax.numpy as jnp
import numpy as np
from jax import lax

MODEL_WIDTH = 2048
HEADS = 32
HEAD = 64
FFE = 3584
TOPK = 2
TOK_DEV = 128
SEQUENCE_TOKENS = 2048
HALF = 64
EXPERTS = 8
CAP = 32


def head_kinds(key):
    order = jax.random.permutation(jax.random.fold_in(key, 101), HEADS)
    slow_count = HEADS // 2
    return jnp.repeat((order < slow_count).astype(jnp.float32), HEAD)


def draw_log_rate(key, part):
    lagging_columns = head_kinds(key)
    sequence_lanes = jax.random.split(jax.random.fold_in(key, 202), 6)
    slow_rate = jnp.exp(jax.random.uniform(sequence_lanes[0], (MODEL_WIDTH,), jnp.float32, math.log(0.2), math.log(0.6))) / SEQUENCE_TOKENS
    fast_rate = jnp.exp(-jax.random.uniform(sequence_lanes[1], (MODEL_WIDTH,), jnp.float32, math.log(30.0), math.log(100.0)))
    base_rate = jnp.where(lagging_columns > 0.5, slow_rate, fast_rate)
    block_factor = jnp.exp(jax.random.uniform(sequence_lanes[2], (SEQUENCE_TOKENS // TOK_DEV, 1), jnp.float32, math.log(0.5), math.log(2.0)))
    block_factor = jnp.repeat(block_factor, TOK_DEV, axis=0)
    jitter = jnp.clip(0.4 * jax.random.normal(sequence_lanes[3], (SEQUENCE_TOKENS, MODEL_WIDTH), jnp.float32), -1.2, 1.2)
    decay_rate_table = base_rate[None, :] * block_factor * jnp.exp(jitter)
    surge_positions = jax.random.randint(sequence_lanes[4], (2,), 0, SEQUENCE_TOKENS)
    surge_decay_loss = -jnp.log(jax.random.uniform(sequence_lanes[5], (2, MODEL_WIDTH), jnp.float32, 0.55, 0.8))
    surge_token_hits = (jnp.arange(SEQUENCE_TOKENS)[:, None] == surge_positions[None, :]).astype(jnp.float32)
    decay_rate_table = decay_rate_table + jnp.dot(surge_token_hits, surge_decay_loss) * lagging_columns[None, :]
    return jnp.clip(jnp.log(decay_rate_table), -14.0, 0.0)


def draw_learn_pre(key, part):
    lagging_columns = head_kinds(key)
    sequence_lanes = jax.random.split(jax.random.fold_in(key, 404), 1)
    jitter = jnp.clip(jax.random.normal(sequence_lanes[0], (SEQUENCE_TOKENS, MODEL_WIDTH), jnp.float32), -4.0, 4.0)
    slow_pre = math.log(0.5 * HEAD / SEQUENCE_TOKENS) + 0.5 * jitter
    return jnp.clip(jnp.where(lagging_columns[None, :] > 0.5, slow_pre, jitter), -12.0, 4.0).astype(jnp.bfloat16)


def level_of(own_key, shape, shards, least, top_value):
    gain = 1.0
    for axis_at, parts in shards:
        steps = jax.random.uniform(jax.random.fold_in(jax.random.fold_in(own_key, 6), axis_at), (parts,), jnp.float32, least / len(shards), top_value / len(shards))
        gain = gain * jnp.repeat(jnp.exp(steps), shape[axis_at] // parts).reshape((-1,) + (1,) * (len(shape) - 1 - axis_at))
    return gain


def deal_out(own_key, own, number, rows, number_of, top, most, slope):
    sequence = jax.random.permutation(own_key, number_of)
    crowded, usual = load_shares(number_of, rows * top, most, slope, True), load_shares(number_of, rows * top, most, slope, False)
    places = jnp.arange(number_of)

    def named(lengths, turn):
        used = int((lengths > 0).sum())
        fixed = max(1, used // 4)
        shifted = fixed + (places - fixed + turn * (used - fixed)) % max(1, number_of - fixed)
        return jnp.zeros((number_of,), jnp.int32).at[sequence[jnp.where(places < fixed, places, shifted)]].set(jnp.asarray(lengths, jnp.int32))

    lengths = jnp.where(number % 4 == 0, named(crowded, number // 4), named(usual, number - number // 4 - 1))
    mixed = jax.random.permutation(jax.random.fold_in(own, 3), number_of)
    source_of, sink = mixed[0:number_of // 2 * 2:2], mixed[1:number_of // 2 * 2:2]
    margin = jnp.minimum(lengths[source_of] - 1, most - lengths[sink]) // 2
    margin = jnp.where((source_of == sequence[0]) | (sink == sequence[0]) | (lengths[sink] == 0), 0, jnp.maximum(margin, 0))
    shifted = jax.random.randint(jax.random.fold_in(own, 4), (number_of // 2,), 0, 1 << 20) % (margin + 1)
    lengths = lengths.at[source_of].add(-shifted).at[sink].add(shifted)
    items = jnp.searchsorted(jnp.cumsum(lengths), jnp.arange(rows * top), side="right").astype(jnp.int32)
    table = items.reshape(top, rows).T
    table = table[jax.random.permutation(jax.random.fold_in(own, 1), rows)]
    turn = jax.random.randint(jax.random.fold_in(own, 2), (rows, 1), 0, top)
    return jnp.take_along_axis(table, (jnp.arange(top)[None, :] + turn) % top, axis=1)


def load_shares(count, total, bound, skew, full):
    weights = [(1 << 20) // math.isqrt(rank ** skew) + 1 for rank in range(1, count + 1)]
    largest = bound if full else min(bound, max(-(-total // count), total * weights[0] // sum(weights)))
    least = 1 if total - largest >= count - 1 else 0
    counts, surplus = [largest] + [least] * (count - 1), total - largest - least * (count - 1)
    while surplus > 0:
        movable = [i for i in range(1, count) if counts[i] < largest] or [i for i in range(1, count) if counts[i] < bound]
        whole, left = sum([weights[i] for i in movable]), surplus
        for i in movable:
            addition = min(bound - counts[i], max(1, left * weights[i] // whole), surplus)
            counts[i] = counts[i] + addition
            surplus = surplus - addition
    return np.array(counts)


def normal_values(rng, dims, deviation, most, cuts=(), held_as=jnp.bfloat16):
    values = jax.random.normal(rng, dims, jnp.float32) * deviation
    if len(cuts) > 0:
        values = level_of(rng, dims, cuts, -0.22, 0.18) * values
    return jnp.clip(values, min=-most, max=most).astype(held_as)


def setup_inputs(seed: int = 0) -> dict:
    streams_of = jax.random.split(jax.random.key(seed), 16)
    stream_in = normal_values(streams_of[0], (SEQUENCE_TOKENS, MODEL_WIDTH), 1.0, 6.0, ((0, 32),))
    query_rows = normal_values(streams_of[1], (SEQUENCE_TOKENS, MODEL_WIDTH), 1.0, 6.0, ((0, 16), (1, 2)))
    key_rows = normal_values(streams_of[2], (SEQUENCE_TOKENS, MODEL_WIDTH), 1.0, 6.0, ((0, 16), (1, 2)))
    value_rows = normal_values(streams_of[3], (SEQUENCE_TOKENS, MODEL_WIDTH), 1.0, 6.0, ((0, 16), (1, 2)))
    removal_key = normal_values(streams_of[4], (SEQUENCE_TOKENS, MODEL_WIDTH), 1.0, 6.0, ((0, 16), (1, 2)))
    learn_pre = draw_learn_pre(jax.random.fold_in(streams_of[15], 71), 0)
    log_rate = draw_log_rate(jax.random.fold_in(streams_of[15], 71), 0)
    norm_gain = jnp.clip(1.0 + 0.18 * jax.random.normal(streams_of[7], (MODEL_WIDTH,), jnp.float32), 0.099609375, 1.8984375).astype(jnp.bfloat16)
    out_weight = normal_values(streams_of[8], (MODEL_WIDTH, MODEL_WIDTH), MODEL_WIDTH ** -0.5, 0.125)
    ffn_gain = jnp.clip(1.0 + 0.18 * jax.random.normal(streams_of[9], (MODEL_WIDTH,), jnp.float32), 0.099609375, 1.8984375).astype(jnp.bfloat16)
    routes_keys = jax.random.split(jax.random.fold_in(streams_of[10], 1), SEQUENCE_TOKENS // HALF)
    routes_turns = jax.random.permutation(jax.random.fold_in(streams_of[10], 3), SEQUENCE_TOKENS // HALF)
    routes = jax.vmap(lambda own, number: deal_out(jax.random.fold_in(streams_of[10], 2), own, number, HALF, EXPERTS, TOPK, CAP, 1))(routes_keys, routes_turns).reshape((SEQUENCE_TOKENS, TOPK))
    route_weight = jnp.clip(0.1 + 0.9 * jax.random.uniform(streams_of[11], (SEQUENCE_TOKENS, TOPK), jnp.float32) ** level_of(streams_of[11], (SEQUENCE_TOKENS, TOPK), ((0, 32),), -0.2, 0.2), 0.1, 1.0)
    expert_gate = normal_values(streams_of[12], (2 * EXPERTS, MODEL_WIDTH, FFE // 2), MODEL_WIDTH ** -0.5, 0.125, ((0, 16), (2, 2)))
    expert_up = normal_values(streams_of[13], (2 * EXPERTS, MODEL_WIDTH, FFE // 2), MODEL_WIDTH ** -0.5, 0.125, ((0, 16), (2, 2)))
    expert_down = normal_values(streams_of[14], (2 * EXPERTS, FFE // 2, MODEL_WIDTH), FFE ** -0.5, 0.09375, ((0, 16), (1, 2)))
    return dict(stream_in=stream_in, query_rows=query_rows, key_rows=key_rows, value_rows=value_rows, removal_key=removal_key, learn_pre=learn_pre, log_rate=log_rate, norm_gain=norm_gain, out_weight=out_weight, ffn_gain=ffn_gain, routes=routes, route_weight=route_weight, expert_gate=expert_gate, expert_up=expert_up, expert_down=expert_down)


HIGH = lax.Precision.HIGHEST
GROUP_EPS = 0.00064
NORM_EPS = 1e-06
UNIT_EPS = 1e-06

def recurrence(carried, inputs):
    queries, key_vals, values, unit_key, pull_key, decays = inputs
    along_unit = jnp.einsum('hvk,hk->hv', carried, unit_key, precision=HIGH)
    carried = carried * decays[:, None, :] - along_unit[:, :, None] * pull_key[:, None, :] + values[:, :, None] * key_vals[:, None, :]
    return (carried, jnp.einsum('hvk,hk->hv', carried, queries, precision=HIGH))

def to_heads(array):
    return array.astype(jnp.float32).reshape(SEQUENCE_TOKENS, HEADS, HEAD)

def expert_rows(routed, gate_pair, up_pair, down_pair):
    quarter = FFE // 4
    running_sum = jnp.zeros((routed.shape[0], MODEL_WIDTH), jnp.float32)
    for half_index in range(2):
        for column_index in range(2):
            start_col = column_index * quarter
            gate_act = jnp.dot(routed, gate_pair[half_index, :, start_col:start_col + quarter], preferred_element_type=jnp.float32)
            up_act = jnp.dot(routed, up_pair[half_index, :, start_col:start_col + quarter], preferred_element_type=jnp.float32)
            hidden = (jax.nn.silu(gate_act) * up_act).astype(jnp.bfloat16)
            partial_out = jnp.dot(hidden, down_pair[half_index, start_col:start_col + quarter, :], preferred_element_type=jnp.float32).astype(jnp.bfloat16)
            running_sum = running_sum + partial_out.astype(jnp.float32)
    return running_sum.astype(jnp.bfloat16)

def reference(stream_in, query_rows, key_rows, value_rows, removal_key, learn_pre, log_rate, norm_gain, out_weight, ffn_gain, routes, route_weight, expert_gate, expert_up, expert_down):
    removal = to_heads(removal_key)
    unit_key = removal / jnp.sqrt(lax.optimization_barrier(jnp.sum(removal * removal, axis=-1, keepdims=True)) + UNIT_EPS)
    pull_key = unit_key * jax.nn.sigmoid(to_heads(learn_pre))
    decays = jnp.exp(-jnp.exp(to_heads(log_rate)))
    initial = jnp.zeros((HEADS, HEAD, HEAD), jnp.float32)
    inputs = (to_heads(query_rows), to_heads(key_rows), to_heads(value_rows), unit_key, pull_key, decays)
    _, mixed = lax.scan(recurrence, initial, inputs)
    centred = mixed - lax.optimization_barrier(jnp.mean(mixed, axis=-1, keepdims=True))
    variance = lax.optimization_barrier(jnp.mean(centred * centred, axis=-1, keepdims=True))
    normed = (centred * lax.rsqrt(variance + GROUP_EPS)).reshape(SEQUENCE_TOKENS, MODEL_WIDTH)
    normed = (normed * norm_gain.astype(jnp.float32)).astype(jnp.bfloat16)
    attended = stream_in.astype(jnp.float32) + jnp.dot(normed, out_weight, preferred_element_type=jnp.float32)
    scaling = lax.rsqrt(lax.optimization_barrier(jnp.mean(attended * attended, axis=-1, keepdims=True)) + NORM_EPS)
    ffn_in = (attended * scaling * ffn_gain.astype(jnp.float32)).astype(jnp.bfloat16)
    sources = SEQUENCE_TOKENS // HALF
    pairs = HALF * TOPK
    expert_ids = routes.reshape(sources, pairs).astype(jnp.int32)
    one_hot = (expert_ids[:, :, None] == jnp.arange(EXPERTS, dtype=jnp.int32)[None, None, :]).astype(jnp.int32)
    slot_index = (lax.optimization_barrier(jnp.sum(jnp.cumsum(one_hot, axis=1) * one_hot, axis=2)) - 1).astype(jnp.int32)
    source_index = jnp.broadcast_to(jnp.arange(sources, dtype=jnp.int32)[:, None], (sources, pairs))
    pair_rows = jnp.repeat(ffn_in.reshape(sources, HALF, MODEL_WIDTH), TOPK, axis=1)
    buffer = jnp.zeros((EXPERTS, sources, CAP, MODEL_WIDTH), jnp.bfloat16)
    buffer = buffer.at[expert_ids, source_index, slot_index].set(pair_rows)

    def run_expert(operands):
        routed, gate_pair, up_pair, down_pair = operands
        outcome = expert_rows(routed.reshape(sources * CAP, MODEL_WIDTH), gate_pair, up_pair, down_pair)
        return outcome.reshape(sources, CAP, MODEL_WIDTH)
    results = lax.map(run_expert, (buffer, expert_gate.reshape(EXPERTS, 2, MODEL_WIDTH, FFE // 2), expert_up.reshape(EXPERTS, 2, MODEL_WIDTH, FFE // 2), expert_down.reshape(EXPERTS, 2, FFE // 2, MODEL_WIDTH)))
    picked = results[expert_ids, source_index, slot_index].astype(jnp.float32)
    weights = route_weight.reshape(sources, pairs)
    mixture = lax.optimization_barrier(jnp.sum((picked * weights[:, :, None]).reshape(sources, HALF, TOPK, MODEL_WIDTH), axis=2))
    return (attended + mixture.reshape(SEQUENCE_TOKENS, MODEL_WIDTH)).astype(jnp.bfloat16)
```

```python
import functools

import jax
import jax.numpy as jnp
from jax import lax
from jax.experimental import pallas as pl
from jax.experimental.pallas import tpu as pltpu
from jax.sharding import PartitionSpec as P

HEAD = 64
TOPK = 2
STEP_HEADS = 4

GROUP_EPS = 0.00064
NORM_EPS = 1e-06
UNIT_EPS = 1e-06
NT = (((1,), (1,)), ((), ()))
NN = (((1,), (0,)), ((), ()))
TN = (((0,), (0,)), ((), ()))


def split(x):
    high = x.astype(jnp.bfloat16)
    return high, (x - high.astype(jnp.float32)).astype(jnp.bfloat16)


def dot1(a, b, dims=NN):
    return lax.dot_general(a, b, dims, preferred_element_type=jnp.float32)


def dot3(a, b, dims=NN):
    return dot1(a[0], b[0], dims) + (dot1(a[0], b[1], dims) + dot1(a[1], b[0], dims))


def mixer_kernel(q_ref, k_ref, v_ref, r_ref, l_ref, g_ref, local_ref, carry_ref, pair_ref):
    tokens = q_ref.shape[0]
    heads = q_ref.shape[1] // HEAD
    row = lax.broadcasted_iota(jnp.int32, (tokens, tokens), 0)
    col = lax.broadcasted_iota(jnp.int32, (tokens, tokens), 1)
    strict = row > col
    upto = row >= col
    eye = (row == col).astype(jnp.float32)
    ones = upto.astype(jnp.bfloat16)
    small_eye = (
        lax.broadcasted_iota(jnp.int32, (HEAD, HEAD), 0)
        == lax.broadcasted_iota(jnp.int32, (HEAD, HEAD), 1)
    ).astype(jnp.float32)
    log_decay = -jnp.exp(g_ref[...])
    high, rest = split(log_decay)
    low = log_decay - high.astype(jnp.float32) - rest.astype(jnp.float32)
    cumul = dot1(ones, high) + (dot1(ones, rest) + dot1(ones, low.astype(jnp.bfloat16)))
    before = cumul - log_decay
    middle = cumul[tokens // 2 - 1 : tokens // 2, :]
    last = cumul[tokens - 1 : tokens, :]
    grow = jnp.exp(middle - cumul)
    fade_now = jnp.exp(cumul - middle)
    fade_prev = jnp.exp(before - middle)
    start_now = jnp.exp(cumul)
    start_prev = jnp.exp(before)
    tail = jnp.exp(last - cumul)
    queries = q_ref[...].astype(jnp.float32)
    keys = k_ref[...].astype(jnp.float32)
    removal = r_ref[...].astype(jnp.float32)
    rate = 1.0 / (1.0 + jnp.exp(-l_ref[...].astype(jnp.float32)))
    locals_out, carries_out = [], []
    state = []
    for h in range(heads):
        at = slice(h * HEAD, (h + 1) * HEAD)
        part = removal[:, at]
        unit = part * lax.rsqrt(jnp.sum(part * part, axis=1, keepdims=True) + UNIT_EPS)
        pull = unit * rate[:, at]
        lefts = jnp.concatenate((unit * fade_prev[:, at], queries[:, at] * fade_now[:, at]), axis=0)
        rights = jnp.concatenate((pull * grow[:, at], keys[:, at] * grow[:, at]), axis=0)
        gram = dot3(split(lefts), split(rights), NT)
        mix_pull = jnp.where(strict, gram[:tokens, :tokens], 0.0)
        mix_key = jnp.where(strict, gram[:tokens, tokens:], 0.0)
        read_pull = jnp.where(upto, gram[tokens:, :tokens], 0.0)
        read_key = jnp.where(upto, gram[tokens:, tokens:], 0.0)
        state.append([unit, pull, mix_pull, mix_key, read_pull, read_key])
    inverses = []
    size = 1
    quads = []
    while size < tokens:
        quads.append((row // (2 * size) == col // (2 * size)) & (row // size > col // size))
        size *= 2
    inverses = [eye - jnp.where(quads[0], one[2], 0.0) for one in state]
    for quad in quads[1:]:
        parts = [split(x) for x in inverses]
        inner = [
            dot3(split(jnp.where(quad, one[2], 0.0)), x) for one, x in zip(state, parts)
        ]
        inverses = [
            x - dot3(p, split(y)) for x, p, y in zip(inverses, parts, inner)
        ]
    for h in range(heads):
        at = slice(h * HEAD, (h + 1) * HEAD)
        unit, pull, mix_pull, mix_key, read_pull, read_key = state[h]
        values = v_ref[:, at]
        mix = split(mix_key)
        read = split(read_key)
        both = jnp.concatenate((mix_key, read_key), axis=0)
        both = split(both)
        both = dot1(both[0], values) + dot1(both[1], values)
        sources = jnp.concatenate((both[:tokens], unit * start_prev[:, at]), axis=1)
        solved = split(dot3(split(inverses[h]), split(sources)))
        taken = dot3(split(read_pull), solved)
        locals_out.append(both[tokens:] - taken[:, :HEAD])
        carries_out.append(queries[:, at] * start_now[:, at] - taken[:, HEAD:])
        left = dot3(solved, split(pull * tail[:, at]), TN)
        key_tail = split(keys[:, at] * tail[:, at])
        grown = dot1(values, key_tail[0], TN) + dot1(values, key_tail[1], TN)
        shift = small_eye * (jnp.exp(last[:, at]) - 1.0) - left[HEAD:]
        pair_ref[h] = jnp.concatenate((shift, grown - left[:HEAD]), axis=1).astype(pair_ref.dtype)
    local_ref[...] = jnp.concatenate(locals_out, axis=1)
    carry_ref[...] = jnp.concatenate(carries_out, axis=1).astype(carry_ref.dtype)


def mix_here(queries, keys, values, removal, learn, rates):
    tokens, width = queries.shape
    lanes = STEP_HEADS * HEAD
    block = pl.BlockSpec((tokens, lanes), lambda i: (0, i))
    return pl.pallas_call(
        mixer_kernel,
        grid=(width // lanes,),
        in_specs=[block] * 6,
        out_specs=[block, block, pl.BlockSpec((STEP_HEADS, HEAD, 2 * HEAD), lambda i: (i, 0, 0))],
        out_shape=[
            jax.ShapeDtypeStruct((tokens, width), jnp.float32),
            jax.ShapeDtypeStruct((tokens, width), jnp.bfloat16),
            jax.ShapeDtypeStruct((width // HEAD, HEAD, 2 * HEAD), jnp.bfloat16),
        ],
        compiler_params=pltpu.CompilerParams(vmem_limit_bytes=60 * 2**20),
    )(queries, keys, values, removal, learn, rates)


def chain_kernel(pair_ref, out_ref):
    state = jnp.zeros((HEAD, HEAD), jnp.float32)
    count = pair_ref.shape[0]
    for k in range(count):
        out_ref[k] = state.astype(out_ref.dtype)
        if k < count - 1:
            shift = pair_ref[k, :, :HEAD]
            high, low = split(state)
            moved = dot1(high, shift) + dot1(low, shift)
            state = state + moved + pair_ref[k, :, HEAD:].astype(jnp.float32)


def entering_state(pairs, axis):
    heads = pairs.shape[0]
    devices = lax.axis_size(axis)
    pieces = devices // heads
    if pieces > 1:
        pairs = jnp.repeat(pairs, pieces, axis=0)
    mine = lax.all_to_all(pairs, axis, split_axis=0, concat_axis=0, tiled=True)
    states = pl.pallas_call(
        chain_kernel,
        out_shape=jax.ShapeDtypeStruct((devices, HEAD, HEAD), jnp.bfloat16),
    )(mine)
    if pieces > 1:
        rows = HEAD // pieces
        states = lax.dynamic_slice_in_dim(states, lax.axis_index(axis) % pieces * rows, rows, 1)
    back = lax.all_to_all(states, axis, split_axis=0, concat_axis=0, tiled=True)
    return back.reshape(heads, HEAD, HEAD)


def finish_kernel(local_ref, carry_ref, state_ref, gain_ref, out_ref):
    outs = []
    for h in range(local_ref.shape[1] // HEAD):
        at = slice(h * HEAD, (h + 1) * HEAD)
        mixed = local_ref[:, at] + dot1(carry_ref[:, at], state_ref[h], NT)
        centred = mixed - jnp.mean(mixed, axis=1, keepdims=True)
        variance = jnp.mean(centred * centred, axis=1, keepdims=True)
        outs.append(centred * lax.rsqrt(variance + GROUP_EPS))
    normed = jnp.concatenate(outs, axis=1) * gain_ref[...].astype(jnp.float32)
    out_ref[...] = normed.astype(jnp.bfloat16)


def finish(local_read, carry_read, states, gain):
    return pl.pallas_call(
        finish_kernel, out_shape=jax.ShapeDtypeStruct(local_read.shape, jnp.bfloat16)
    )(local_read, carry_read, states, gain[None, :])


def from_partner(array, axis, bit):
    return lax.ppermute(array, axis, [(i, i ^ 1 << bit) for i in range(lax.axis_size(axis))])


def local(
    stream_in,
    query_rows,
    key_rows,
    value_rows,
    removal_key,
    learn_pre,
    log_rate,
    norm_gain,
    out_weight,
    ffn_gain,
    routes,
    route_weight,
    expert_gate,
    expert_up,
    expert_down,
):
    local_read, carry_read, pairs = mix_here(
        query_rows, key_rows, value_rows, removal_key, learn_pre, log_rate
    )
    states = entering_state(pairs, "sp")
    normed = finish(local_read, carry_read, states, norm_gain)
    gathered = lax.all_to_all(normed, "tp", split_axis=0, concat_axis=1, tiled=True)
    attended = stream_in.astype(jnp.float32) + jnp.dot(
        gathered, out_weight, preferred_element_type=jnp.float32
    )
    scaling = lax.rsqrt(jnp.mean(attended * attended, axis=-1, keepdims=True) + NORM_EPS)
    ffn_in = (attended * scaling * ffn_gain.astype(jnp.float32)).astype(jnp.bfloat16)
    half_rows = attended.shape[0]
    width = attended.shape[1]
    experts = lax.axis_size("sp") // 2
    peers = lax.axis_size("sp") * lax.axis_size("tp")
    capacity = 2 * TOPK * half_rows // experts
    pairs = half_rows * TOPK
    expert_ids = routes.reshape(pairs)
    one_hot = (expert_ids[:, None] == jnp.arange(experts, dtype=jnp.int32)[None, :]).astype(
        jnp.int32
    )
    slot_index = jnp.sum(jnp.cumsum(one_hot, axis=0) * one_hot, axis=1) - 1
    send_index = expert_ids * capacity + slot_index
    send_map = (
        jnp.arange(experts * capacity, dtype=jnp.int32)[:, None] == send_index[None, :]
    ).astype(jnp.bfloat16)
    send_map = jnp.sum(send_map.reshape(experts * capacity, half_rows, TOPK), axis=2)
    dispatched = jnp.dot(send_map, ffn_in, preferred_element_type=jnp.float32).astype(jnp.bfloat16)
    quarters = lax.all_to_all(dispatched, ("sp", "tp"), split_axis=0, concat_axis=0, tiled=True)
    quarters = quarters.reshape(peers, capacity // 4, width)
    partner = from_partner(quarters, "sp", 0)
    even = lax.axis_index("sp") % 2 == 0
    both_chips = jnp.stack((jnp.where(even, quarters, partner), jnp.where(even, partner, quarters)))
    routed = lax.all_gather(both_chips, "tp", axis=2, tiled=True)
    routed = routed.transpose(1, 0, 2, 3).reshape(peers * capacity, width)
    gate_act = jnp.dot(routed, expert_gate[0], preferred_element_type=jnp.float32)
    up_act = jnp.dot(routed, expert_up[0], preferred_element_type=jnp.float32)
    hidden = (jax.nn.silu(gate_act) * up_act).astype(jnp.bfloat16)
    partial_out = jnp.dot(hidden, expert_down[0], preferred_element_type=jnp.float32).astype(
        jnp.bfloat16
    )
    partial_out = partial_out.reshape(peers, capacity, width)
    pair_bit = lax.axis_index("sp") % 2
    core_sum = lax.psum_scatter(partial_out, "tp", scatter_dimension=2, tiled=True)
    part_width = core_sum.shape[2] // 2
    kept = lax.dynamic_slice_in_dim(core_sum, pair_bit * part_width, part_width, 2)
    sent = lax.dynamic_slice_in_dim(core_sum, (1 - pair_bit) * part_width, part_width, 2)
    arrived = from_partner(sent, "sp", 0)
    expert_out = (kept.astype(jnp.float32) + arrived.astype(jnp.float32)).astype(jnp.bfloat16)
    returned = lax.all_to_all(expert_out, ("sp", "tp"), split_axis=0, concat_axis=2, tiled=True)
    returned = returned.reshape(capacity * experts, width)
    back_index = slot_index * experts + expert_ids
    back_map = (
        back_index[:, None] == jnp.arange(capacity * experts, dtype=jnp.int32)[None, :]
    ).astype(jnp.bfloat16)
    picked = jnp.dot(back_map, returned, preferred_element_type=jnp.float32).reshape(
        half_rows, TOPK, width
    )
    mixture = jnp.sum(picked * route_weight[:, :, None], axis=1)
    quarters = jnp.split(mixture, 4, axis=1)
    mixture = jnp.concatenate((quarters[0], quarters[2], quarters[1], quarters[3]), axis=1)
    return (attended + mixture).astype(jnp.bfloat16)


def solution(mesh):
    placed = (
        P(("sp", "tp"), None),
        P("sp", "tp"),
        P("sp", "tp"),
        P("sp", "tp"),
        P("sp", "tp"),
        P("sp", "tp"),
        P("sp", "tp"),
        P("tp"),
        P(),
        P(),
        P(("sp", "tp"), None),
        P(("sp", "tp"), None),
        P("sp", None, "tp"),
        P("sp", None, "tp"),
        P("sp", "tp", None),
    )
    return jax.shard_map(
        local, mesh=mesh, in_specs=placed, out_specs=P(("sp", "tp"), None), check_vma=False
    )
```

```python
import functools

import jax
import jax.numpy as jnp
from jax import lax
from jax.experimental import pallas as pl
from jax.experimental.pallas import tpu as pltpu
from jax.sharding import PartitionSpec as P

HEAD = 64
TOPK = 2
STEP_HEADS = 4

GROUP_EPS = 0.00064
NORM_EPS = 1e-06
UNIT_EPS = 1e-06
NT = (((1,), (1,)), ((), ()))
NN = (((1,), (0,)), ((), ()))
TN = (((0,), (0,)), ((), ()))


def split(x):
    high = x.astype(jnp.bfloat16)
    return high, (x - high.astype(jnp.float32)).astype(jnp.bfloat16)


def dot1(a, b, dims=NN):
    return lax.dot_general(a, b, dims, preferred_element_type=jnp.float32)


def dot3(a, b, dims=NN):
    return dot1(a[0], b[0], dims) + (dot1(a[0], b[1], dims) + dot1(a[1], b[0], dims))


def mixer_kernel(q_ref, k_ref, v_ref, r_ref, l_ref, g_ref, local_ref, carry_ref, pair_ref):
    tokens = q_ref.shape[0]
    heads = q_ref.shape[1] // HEAD
    row = lax.broadcasted_iota(jnp.int32, (tokens, tokens), 0)
    col = lax.broadcasted_iota(jnp.int32, (tokens, tokens), 1)
    strict = row > col
    upto = row >= col
    eye = (row == col).astype(jnp.float32)
    ones = upto.astype(jnp.bfloat16)
    small_eye = (
        lax.broadcasted_iota(jnp.int32, (HEAD, HEAD), 0)
        == lax.broadcasted_iota(jnp.int32, (HEAD, HEAD), 1)
    ).astype(jnp.float32)
    log_decay = -jnp.exp(g_ref[...])
    high, rest = split(log_decay)
    low = log_decay - high.astype(jnp.float32) - rest.astype(jnp.float32)
    cumul = dot1(ones, high) + (dot1(ones, rest) + dot1(ones, low.astype(jnp.bfloat16)))
    before = cumul - log_decay
    middle = cumul[tokens // 2 - 1 : tokens // 2, :]
    last = cumul[tokens - 1 : tokens, :]
    grow = jnp.exp(middle - cumul)
    fade_now = jnp.exp(cumul - middle)
    fade_prev = jnp.exp(before - middle)
    start_now = jnp.exp(cumul)
    start_prev = jnp.exp(before)
    tail = jnp.exp(last - cumul)
    queries = q_ref[...].astype(jnp.float32)
    keys = k_ref[...].astype(jnp.float32)
    removal = r_ref[...].astype(jnp.float32)
    rate = 1.0 / (1.0 + jnp.exp(-l_ref[...].astype(jnp.float32)))
    locals_out, carries_out = [], []
    state = []
    for h in range(heads):
        at = slice(h * HEAD, (h + 1) * HEAD)
        part = removal[:, at]
        unit = part * lax.rsqrt(jnp.sum(part * part, axis=1, keepdims=True) + UNIT_EPS)
        pull = unit * rate[:, at]
        lefts = jnp.concatenate((unit * fade_prev[:, at], queries[:, at] * fade_now[:, at]), axis=0)
        rights = jnp.concatenate((pull * grow[:, at], keys[:, at] * grow[:, at]), axis=0)
        gram = dot3(split(lefts), split(rights), NT)
        mix_pull = jnp.where(strict, gram[:tokens, :tokens], 0.0)
        mix_key = jnp.where(strict, gram[:tokens, tokens:], 0.0)
        read_pull = jnp.where(upto, gram[tokens:, :tokens], 0.0)
        read_key = jnp.where(upto, gram[tokens:, tokens:], 0.0)
        state.append([unit, pull, mix_pull, mix_key, read_pull, read_key])
    inverses = []
    size = 1
    quads = []
    while size < tokens:
        quads.append((row // (2 * size) == col // (2 * size)) & (row // size > col // size))
        size *= 2
    inverses = [eye - jnp.where(quads[0], one[2], 0.0) for one in state]
    for quad in quads[1:]:
        parts = [split(x) for x in inverses]
        inner = [
            dot3(split(jnp.where(quad, one[2], 0.0)), x) for one, x in zip(state, parts)
        ]
        inverses = [
            x - dot3(p, split(y)) for x, p, y in zip(inverses, parts, inner)
        ]
    for h in range(heads):
        at = slice(h * HEAD, (h + 1) * HEAD)
        unit, pull, mix_pull, mix_key, read_pull, read_key = state[h]
        values = v_ref[:, at]
        mix = split(mix_key)
        read = split(read_key)
        both = jnp.concatenate((mix_key, read_key), axis=0)
        both = split(both)
        both = dot1(both[0], values) + dot1(both[1], values)
        sources = jnp.concatenate((both[:tokens], unit * start_prev[:, at]), axis=1)
        solved = split(dot3(split(inverses[h]), split(sources)))
        taken = dot3(split(read_pull), solved)
        locals_out.append(both[tokens:] - taken[:, :HEAD])
        carries_out.append(queries[:, at] * start_now[:, at] - taken[:, HEAD:])
        left = dot3(solved, split(pull * tail[:, at]), TN)
        key_tail = split(keys[:, at] * tail[:, at])
        grown = dot1(values, key_tail[0], TN) + dot1(values, key_tail[1], TN)
        shift = small_eye * (jnp.exp(last[:, at]) - 1.0) - left[HEAD:]
        pair_ref[h] = jnp.concatenate((shift, grown - left[:HEAD]), axis=1).astype(pair_ref.dtype)
    local_ref[...] = jnp.concatenate(locals_out, axis=1)
    carry_ref[...] = jnp.concatenate(carries_out, axis=1).astype(carry_ref.dtype)


def mix_here(queries, keys, values, removal, learn, rates):
    tokens, width = queries.shape
    lanes = STEP_HEADS * HEAD
    block = pl.BlockSpec((tokens, lanes), lambda i: (0, i))
    return pl.pallas_call(
        mixer_kernel,
        grid=(width // lanes,),
        in_specs=[block] * 6,
        out_specs=[block, block, pl.BlockSpec((STEP_HEADS, HEAD, 2 * HEAD), lambda i: (i, 0, 0))],
        out_shape=[
            jax.ShapeDtypeStruct((tokens, width), jnp.float32),
            jax.ShapeDtypeStruct((tokens, width), jnp.bfloat16),
            jax.ShapeDtypeStruct((width // HEAD, HEAD, 2 * HEAD), jnp.bfloat16),
        ],
        compiler_params=pltpu.CompilerParams(vmem_limit_bytes=60 * 2**20),
    )(queries, keys, values, removal, learn, rates)


def chain_kernel(pair_ref, out_ref):
    state = jnp.zeros((HEAD, HEAD), jnp.float32)
    count = pair_ref.shape[0]
    for k in range(count):
        out_ref[k] = state.astype(out_ref.dtype)
        if k < count - 1:
            shift = pair_ref[k, :, :HEAD]
            high, low = split(state)
            moved = dot1(high, shift) + dot1(low, shift)
            state = state + moved + pair_ref[k, :, HEAD:].astype(jnp.float32)


def entering_state(pairs, axis):
    heads = pairs.shape[0]
    devices = lax.axis_size(axis)
    pieces = devices // heads
    if pieces > 1:
        pairs = jnp.repeat(pairs, pieces, axis=0)
    mine = lax.all_to_all(pairs, axis, split_axis=0, concat_axis=0, tiled=True)
    states = pl.pallas_call(
        chain_kernel,
        out_shape=jax.ShapeDtypeStruct((devices, HEAD, HEAD), jnp.bfloat16),
    )(mine)
    if pieces > 1:
        rows = HEAD // pieces
        states = lax.dynamic_slice_in_dim(states, lax.axis_index(axis) % pieces * rows, rows, 1)
    back = lax.all_to_all(states, axis, split_axis=0, concat_axis=0, tiled=True)
    return back.reshape(heads, HEAD, HEAD)


def finish_kernel(local_ref, carry_ref, state_ref, gain_ref, out_ref):
    outs = []
    for h in range(local_ref.shape[1] // HEAD):
        at = slice(h * HEAD, (h + 1) * HEAD)
        mixed = local_ref[:, at] + dot1(carry_ref[:, at], state_ref[h], NT)
        centred = mixed - jnp.mean(mixed, axis=1, keepdims=True)
        variance = jnp.mean(centred * centred, axis=1, keepdims=True)
        outs.append(centred * lax.rsqrt(variance + GROUP_EPS))
    normed = jnp.concatenate(outs, axis=1) * gain_ref[...].astype(jnp.float32)
    out_ref[...] = normed.astype(jnp.bfloat16)


def finish(local_read, carry_read, states, gain):
    return pl.pallas_call(
        finish_kernel, out_shape=jax.ShapeDtypeStruct(local_read.shape, jnp.bfloat16)
    )(local_read, carry_read, states, gain[None, :])


MESH = pl.DeviceIdType.MESH


def places():
    sp, core = lax.axis_index("sp"), lax.axis_index("tp")
    group, side = sp // 2, sp % 2
    return sp, core, group, side


def greet(groups, sp, core, group, side):
    barrier = pltpu.get_barrier_semaphore()
    others = [((group + o) % groups * 2 + side, core) for o in range(1, groups)]
    others += [(group * 2 + 1 - side, core), (sp, 1 - core)]
    for other in others:
        pl.semaphore_signal(barrier, inc=1, device_id=other, device_id_type=MESH)
    pl.semaphore_wait(barrier, len(others))


def remote(source, target, send, recv, device):
    return pltpu.make_async_remote_copy(
        src_ref=source,
        dst_ref=target,
        send_sem=send,
        recv_sem=recv,
        device_id=device,
        device_id_type=MESH,
    )


def dispatch_kernel(rows_ref, out_ref, own_sem, send_sem, recv_sem):
    groups = rows_ref.shape[0]
    sp, core, group, side = places()
    across, beside = (group * 2 + 1 - side, core), (sp, 1 - core)
    greet(groups, sp, core, group, side)
    own = pltpu.make_async_copy(rows_ref.at[group], out_ref.at[group, side, core], own_sem)
    own.start()
    first = {}
    for o in range(1, groups):
        to = (group + o) % groups
        first[o] = remote(
            rows_ref.at[to],
            out_ref.at[group, side, core],
            send_sem.at[0, o],
            recv_sem.at[0, o],
            (to * 2 + side, core),
        )
        first[o].start()
    over, near, last = {}, {}, {}
    lag = 2
    for o in range(groups + lag):
        if o < groups:
            source = (group + groups - o) % groups
            if o == 0:
                own.wait()
            else:
                first[o].wait_recv()
            block = out_ref.at[source, side, core]
            over[o] = remote(block, block, send_sem.at[1, o], recv_sem.at[1, o], across)
            near[o] = remote(block, block, send_sem.at[2, o], recv_sem.at[2, o], beside)
            over[o].start()
            near[o].start()
        if o >= lag:
            p = o - lag
            source = (group + groups - p) % groups
            over[p].wait_recv()
            block = out_ref.at[source, 1 - side, core]
            last[p] = remote(block, block, send_sem.at[3, p], recv_sem.at[3, p], beside)
            last[p].start()
    for o in range(groups):
        near[o].wait_recv()
        last[o].wait_recv()
        if o > 0:
            first[o].wait_send()
        over[o].wait_send()
        near[o].wait_send()
        last[o].wait_send()


def dispatch(rows):
    groups, capacity, width = rows.shape
    return pl.pallas_call(
        dispatch_kernel,
        out_shape=jax.ShapeDtypeStruct((groups, 2, 2, capacity, width), rows.dtype),
        in_specs=[pl.BlockSpec(memory_space=pltpu.VMEM)],
        out_specs=pl.BlockSpec(memory_space=pltpu.VMEM),
        scratch_shapes=[
            pltpu.SemaphoreType.DMA,
            pltpu.SemaphoreType.DMA((4, groups)),
            pltpu.SemaphoreType.DMA((4, groups)),
        ],
        compiler_params=pltpu.CompilerParams(
            collective_id=0, has_side_effects=True, vmem_limit_bytes=40 * 2**20
        ),
    )(rows)


def add(a, b):
    return a.astype(jnp.float32) + b.astype(jnp.float32)


def give_back_kernel(part_ref, out_ref, core_in, core_sum, side_in, total, send_sem, recv_sem):
    groups = part_ref.shape[0]
    sp, core, group, side = places()
    across, beside = (group * 2 + 1 - side, core), (sp, 1 - core)
    greet(groups, sp, core, group, side)
    order = list(range(1, groups)) + [0]
    cores, sides, finals = {}, {}, {}
    for kind, which in ((0, 1 - side), (1, side)):
        for o in order:
            to = (group + o) % groups
            cores[kind, o] = remote(
                part_ref.at[to, which, 1 - core],
                core_in.at[to, which],
                send_sem.at[kind, o],
                recv_sem.at[kind, o],
                beside,
            )
            cores[kind, o].start()
    for o in order:
        to = (group + o) % groups
        cores[0, o].wait_recv()
        core_sum[to] = add(part_ref[to, 1 - side, core], core_in[to, 1 - side]).astype(core_sum.dtype)
        sides[o] = remote(
            core_sum.at[to], side_in.at[to], send_sem.at[2, o], recv_sem.at[2, o], across
        )
        sides[o].start()
    for o in order:
        to = (group + o) % groups
        cores[1, o].wait_recv()
        sides[o].wait_recv()
        kept = add(part_ref[to, side, core], core_in[to, side])
        summed = (kept + side_in[to].astype(jnp.float32)).astype(total.dtype)
        if o == 0:
            out_ref[to] = summed
        else:
            total[to] = summed
            finals[o] = remote(
                total.at[to],
                out_ref.at[group],
                send_sem.at[3, o],
                recv_sem.at[3, o],
                (to * 2 + side, core),
            )
            finals[o].start()
    for o in order:
        if o > 0:
            finals[o].wait()
        sides[o].wait_send()
        cores[0, o].wait_send()
        cores[1, o].wait_send()


def give_back(parts):
    groups, _, _, capacity, width = parts.shape
    block = (groups, capacity, width)
    return pl.pallas_call(
        give_back_kernel,
        out_shape=jax.ShapeDtypeStruct(block, parts.dtype),
        in_specs=[pl.BlockSpec(memory_space=pltpu.VMEM)],
        out_specs=pl.BlockSpec(memory_space=pltpu.VMEM),
        scratch_shapes=[
            pltpu.VMEM((groups, 2, capacity, width), parts.dtype),
            pltpu.VMEM(block, parts.dtype),
            pltpu.VMEM(block, parts.dtype),
            pltpu.VMEM(block, parts.dtype),
            pltpu.SemaphoreType.DMA((4, groups)),
            pltpu.SemaphoreType.DMA((4, groups)),
        ],
        compiler_params=pltpu.CompilerParams(
            collective_id=1, has_side_effects=True, vmem_limit_bytes=40 * 2**20
        ),
    )(parts)


def local(
    stream_in,
    query_rows,
    key_rows,
    value_rows,
    removal_key,
    learn_pre,
    log_rate,
    norm_gain,
    out_weight,
    ffn_gain,
    routes,
    route_weight,
    expert_gate,
    expert_up,
    expert_down,
):
    local_read, carry_read, pairs = mix_here(
        query_rows, key_rows, value_rows, removal_key, learn_pre, log_rate
    )
    states = entering_state(pairs, "sp")
    normed = finish(local_read, carry_read, states, norm_gain)
    gathered = lax.all_to_all(normed, "tp", split_axis=0, concat_axis=1, tiled=True)
    attended = stream_in.astype(jnp.float32) + jnp.dot(
        gathered, out_weight, preferred_element_type=jnp.float32
    )
    scaling = lax.rsqrt(jnp.mean(attended * attended, axis=-1, keepdims=True) + NORM_EPS)
    ffn_in = (attended * scaling * ffn_gain.astype(jnp.float32)).astype(jnp.bfloat16)
    half_rows = attended.shape[0]
    width = attended.shape[1]
    experts = lax.axis_size("sp") // 2
    peers = lax.axis_size("sp") * lax.axis_size("tp")
    capacity = 2 * TOPK * half_rows // experts
    pairs = half_rows * TOPK
    expert_ids = routes.reshape(pairs)
    one_hot = (expert_ids[:, None] == jnp.arange(experts, dtype=jnp.int32)[None, :]).astype(
        jnp.int32
    )
    slot_index = jnp.sum(jnp.cumsum(one_hot, axis=0) * one_hot, axis=1) - 1
    send_index = expert_ids * capacity + slot_index
    send_map = (
        jnp.arange(experts * capacity, dtype=jnp.int32)[:, None] == send_index[None, :]
    ).astype(jnp.bfloat16)
    send_map = jnp.sum(send_map.reshape(experts * capacity, half_rows, TOPK), axis=2)
    dispatched = jnp.dot(send_map, ffn_in, preferred_element_type=jnp.float32).astype(jnp.bfloat16)
    arrived = dispatch(dispatched.reshape(experts, capacity, width))
    routed = arrived.reshape(peers * capacity, width)
    gate_act = jnp.dot(routed, expert_gate[0], preferred_element_type=jnp.float32)
    up_act = jnp.dot(routed, expert_up[0], preferred_element_type=jnp.float32)
    hidden = (jax.nn.silu(gate_act) * up_act).astype(jnp.bfloat16)
    partial_out = jnp.dot(hidden, expert_down[0], preferred_element_type=jnp.float32).astype(
        jnp.bfloat16
    )
    returned = give_back(partial_out.reshape(arrived.shape)).reshape(experts * capacity, width)
    back_map = (
        send_index[:, None] == jnp.arange(experts * capacity, dtype=jnp.int32)[None, :]
    ).astype(jnp.bfloat16)
    picked = jnp.dot(back_map, returned, preferred_element_type=jnp.float32).reshape(
        half_rows, TOPK, width
    )
    mixture = jnp.sum(picked * route_weight[:, :, None], axis=1)
    return (attended + mixture).astype(jnp.bfloat16)


def solution(mesh):
    placed = (
        P(("sp", "tp"), None),
        P("sp", "tp"),
        P("sp", "tp"),
        P("sp", "tp"),
        P("sp", "tp"),
        P("sp", "tp"),
        P("sp", "tp"),
        P("tp"),
        P(),
        P(),
        P(("sp", "tp"), None),
        P(("sp", "tp"), None),
        P("sp", None, "tp"),
        P("sp", None, "tp"),
        P("sp", "tp", None),
    )
    return jax.shard_map(
        local, mesh=mesh, in_specs=placed, out_specs=P(("sp", "tp"), None), check_vma=False
    )
```

```python
import functools

import jax
import jax.numpy as jnp
from jax import lax
from jax.experimental import pallas as pl
from jax.experimental.pallas import tpu as pltpu
from jax.sharding import PartitionSpec as P

HEAD = 64
TOPK = 2
STEP_HEADS = 4

GROUP_EPS = 0.00064
NORM_EPS = 1e-06
UNIT_EPS = 1e-06
NT = (((1,), (1,)), ((), ()))
NN = (((1,), (0,)), ((), ()))
TN = (((0,), (0,)), ((), ()))


def split(x):
    high = x.astype(jnp.bfloat16)
    return high, (x - high.astype(jnp.float32)).astype(jnp.bfloat16)


def dot1(a, b, dims=NN):
    return lax.dot_general(a, b, dims, preferred_element_type=jnp.float32)


def dot3(a, b, dims=NN):
    if dims is NN:
        wide = jnp.concatenate(b, axis=1)
        both = dot1(jnp.concatenate(a, axis=1), jnp.concatenate((wide, wide), axis=0))
        half = both.shape[1] // 2
        return both[:, :half] + both[:, half:]
    return dot1(a[0], b[0], dims) + (dot1(a[0], b[1], dims) + dot1(a[1], b[0], dims))


def mixer_kernel(q_ref, k_ref, v_ref, r_ref, l_ref, g_ref, local_ref, carry_ref, pair_ref):
    tokens = q_ref.shape[0]
    heads = q_ref.shape[1] // HEAD
    row = lax.broadcasted_iota(jnp.int32, (tokens, tokens), 0)
    col = lax.broadcasted_iota(jnp.int32, (tokens, tokens), 1)
    strict = row > col
    upto = row >= col
    eye = (row == col).astype(jnp.float32)
    ones = upto.astype(jnp.bfloat16)
    small_eye = (
        lax.broadcasted_iota(jnp.int32, (HEAD, HEAD), 0)
        == lax.broadcasted_iota(jnp.int32, (HEAD, HEAD), 1)
    ).astype(jnp.float32)
    log_decay = -jnp.exp(g_ref[...])
    high, rest = split(log_decay)
    low = log_decay - high.astype(jnp.float32) - rest.astype(jnp.float32)
    cumul = dot1(ones, high) + (dot1(ones, rest) + dot1(ones, low.astype(jnp.bfloat16)))
    before = cumul - log_decay
    middle = cumul[tokens // 2 - 1 : tokens // 2, :]
    last = cumul[tokens - 1 : tokens, :]
    grow = jnp.exp(middle - cumul)
    fade_now = jnp.exp(cumul - middle)
    fade_prev = jnp.exp(before - middle)
    start_now = jnp.exp(cumul)
    start_prev = jnp.exp(before)
    tail = jnp.exp(last - cumul)
    queries = q_ref[...].astype(jnp.float32)
    keys = k_ref[...].astype(jnp.float32)
    removal = r_ref[...].astype(jnp.float32)
    rate = 1.0 / (1.0 + jnp.exp(-l_ref[...].astype(jnp.float32)))
    locals_out, carries_out = [], []
    state = []
    for h in range(heads):
        at = slice(h * HEAD, (h + 1) * HEAD)
        part = removal[:, at]
        unit = part * lax.rsqrt(jnp.sum(part * part, axis=1, keepdims=True) + UNIT_EPS)
        pull = unit * rate[:, at]
        lefts = jnp.concatenate((unit * fade_prev[:, at], queries[:, at] * fade_now[:, at]), axis=0)
        rights = jnp.concatenate((pull * grow[:, at], keys[:, at] * grow[:, at]), axis=0)
        gram = dot3(split(lefts), split(rights), NT)
        mix_pull = jnp.where(strict, gram[:tokens, :tokens], 0.0)
        mix_key = jnp.where(strict, gram[:tokens, tokens:], 0.0)
        read_pull = jnp.where(upto, gram[tokens:, :tokens], 0.0)
        read_key = jnp.where(upto, gram[tokens:, tokens:], 0.0)
        state.append([unit, pull, mix_pull, mix_key, read_pull, read_key])
    inverses = []
    size = 1
    quads = []
    while size < tokens:
        quads.append((row // (2 * size) == col // (2 * size)) & (row // size > col // size))
        size *= 2
    inverses = [eye - jnp.where(quads[0], one[2], 0.0) for one in state]
    for quad in quads[1:]:
        parts = [split(x) for x in inverses]
        inner = [
            dot3(split(jnp.where(quad, one[2], 0.0)), x) for one, x in zip(state, parts)
        ]
        inverses = [
            x - dot3(p, split(y)) for x, p, y in zip(inverses, parts, inner)
        ]
    for h in range(heads):
        at = slice(h * HEAD, (h + 1) * HEAD)
        unit, pull, mix_pull, mix_key, read_pull, read_key = state[h]
        values = v_ref[:, at]
        mix = split(mix_key)
        read = split(read_key)
        both = jnp.concatenate((mix_key, read_key), axis=0)
        both = split(both)
        both = dot1(both[0], values) + dot1(both[1], values)
        sources = jnp.concatenate((both[:tokens], unit * start_prev[:, at]), axis=1)
        solved = split(dot3(split(inverses[h]), split(sources)))
        taken = dot3(split(read_pull), solved)
        locals_out.append(both[tokens:] - taken[:, :HEAD])
        carries_out.append(queries[:, at] * start_now[:, at] - taken[:, HEAD:])
        left = dot3(solved, split(pull * tail[:, at]), TN)
        key_tail = split(keys[:, at] * tail[:, at])
        grown = dot1(values, key_tail[0], TN) + dot1(values, key_tail[1], TN)
        shift = small_eye * (jnp.exp(last[:, at]) - 1.0) - left[HEAD:]
        pair_ref[h] = jnp.concatenate((shift, grown - left[:HEAD]), axis=1).astype(pair_ref.dtype)
    local_ref[...] = jnp.concatenate(locals_out, axis=1)
    carry_ref[...] = jnp.concatenate(carries_out, axis=1).astype(carry_ref.dtype)


def mix_here(queries, keys, values, removal, learn, rates):
    tokens, width = queries.shape
    lanes = STEP_HEADS * HEAD
    block = pl.BlockSpec((tokens, lanes), lambda i: (0, i))
    return pl.pallas_call(
        mixer_kernel,
        grid=(width // lanes,),
        in_specs=[block] * 6,
        out_specs=[block, block, pl.BlockSpec((STEP_HEADS, HEAD, 2 * HEAD), lambda i: (i, 0, 0))],
        out_shape=[
            jax.ShapeDtypeStruct((tokens, width), jnp.float32),
            jax.ShapeDtypeStruct((tokens, width), jnp.bfloat16),
            jax.ShapeDtypeStruct((width // HEAD, HEAD, 2 * HEAD), jnp.bfloat16),
        ],
        compiler_params=pltpu.CompilerParams(vmem_limit_bytes=60 * 2**20),
    )(queries, keys, values, removal, learn, rates)


def chain_kernel(pair_ref, out_ref):
    state = jnp.zeros((HEAD, HEAD), jnp.float32)
    count = pair_ref.shape[0]
    for k in range(count):
        out_ref[k] = state.astype(out_ref.dtype)
        if k < count - 1:
            shift = pair_ref[k, :, :HEAD]
            high, low = split(state)
            moved = dot1(high, shift) + dot1(low, shift)
            state = state + moved + pair_ref[k, :, HEAD:].astype(jnp.float32)


def entering_state(pairs, axis):
    heads = pairs.shape[0]
    devices = lax.axis_size(axis)
    pieces = devices // heads
    if pieces > 1:
        pairs = jnp.repeat(pairs, pieces, axis=0)
    mine = lax.all_to_all(pairs, axis, split_axis=0, concat_axis=0, tiled=True)
    states = pl.pallas_call(
        chain_kernel,
        out_shape=jax.ShapeDtypeStruct((devices, HEAD, HEAD), jnp.bfloat16),
    )(mine)
    if pieces > 1:
        rows = HEAD // pieces
        states = lax.dynamic_slice_in_dim(states, lax.axis_index(axis) % pieces * rows, rows, 1)
    back = lax.all_to_all(states, axis, split_axis=0, concat_axis=0, tiled=True)
    return back.reshape(heads, HEAD, HEAD)


def finish_kernel(local_ref, carry_ref, state_ref, gain_ref, out_ref):
    outs = []
    for h in range(local_ref.shape[1] // HEAD):
        at = slice(h * HEAD, (h + 1) * HEAD)
        mixed = local_ref[:, at] + dot1(carry_ref[:, at], state_ref[h], NT)
        centred = mixed - jnp.mean(mixed, axis=1, keepdims=True)
        variance = jnp.mean(centred * centred, axis=1, keepdims=True)
        outs.append(centred * lax.rsqrt(variance + GROUP_EPS))
    normed = jnp.concatenate(outs, axis=1) * gain_ref[...].astype(jnp.float32)
    out_ref[...] = normed.astype(jnp.bfloat16)


def finish(local_read, carry_read, states, gain):
    return pl.pallas_call(
        finish_kernel, out_shape=jax.ShapeDtypeStruct(local_read.shape, jnp.bfloat16)
    )(local_read, carry_read, states, gain[None, :])


MESH = pl.DeviceIdType.MESH


def places():
    sp, core = lax.axis_index("sp"), lax.axis_index("tp")
    group, side = sp // 2, sp % 2
    return sp, core, group, side


def greet(groups, sp, core, group, side):
    barrier = pltpu.get_barrier_semaphore()
    others = [((group + o) % groups * 2 + side, core) for o in range(1, groups)]
    others += [(group * 2 + 1 - side, core), (sp, 1 - core)]
    for other in others:
        pl.semaphore_signal(barrier, inc=1, device_id=other, device_id_type=MESH)
    pl.semaphore_wait(barrier, len(others))


def remote(source, target, send, recv, device):
    return pltpu.make_async_remote_copy(
        src_ref=source,
        dst_ref=target,
        send_sem=send,
        recv_sem=recv,
        device_id=device,
        device_id_type=MESH,
    )


def dispatch_kernel(rows_ref, out_ref, own_sem, send_sem, recv_sem):
    groups = rows_ref.shape[0]
    sp, core, group, side = places()
    across, beside = (group * 2 + 1 - side, core), (sp, 1 - core)
    greet(groups, sp, core, group, side)
    own = pltpu.make_async_copy(rows_ref.at[group], out_ref.at[group, side, core], own_sem)
    own.start()
    first = {}
    for o in range(1, groups):
        to = (group + o) % groups
        first[o] = remote(
            rows_ref.at[to],
            out_ref.at[group, side, core],
            send_sem.at[0, o],
            recv_sem.at[0, o],
            (to * 2 + side, core),
        )
        first[o].start()
    over, near, last = {}, {}, {}
    lag = 2
    for o in range(groups + lag):
        if o < groups:
            source = (group + groups - o) % groups
            if o == 0:
                own.wait()
            else:
                first[o].wait_recv()
            block = out_ref.at[source, side, core]
            over[o] = remote(block, block, send_sem.at[1, o], recv_sem.at[1, o], across)
            near[o] = remote(block, block, send_sem.at[2, o], recv_sem.at[2, o], beside)
            over[o].start()
            near[o].start()
        if o >= lag:
            p = o - lag
            source = (group + groups - p) % groups
            over[p].wait_recv()
            block = out_ref.at[source, 1 - side, core]
            last[p] = remote(block, block, send_sem.at[3, p], recv_sem.at[3, p], beside)
            last[p].start()
    for o in range(groups):
        near[o].wait_recv()
        last[o].wait_recv()
        if o > 0:
            first[o].wait_send()
        over[o].wait_send()
        near[o].wait_send()
        last[o].wait_send()


def dispatch(rows):
    groups, capacity, width = rows.shape
    return pl.pallas_call(
        dispatch_kernel,
        out_shape=jax.ShapeDtypeStruct((groups, 2, 2, capacity, width), rows.dtype),
        in_specs=[pl.BlockSpec(memory_space=pltpu.VMEM)],
        out_specs=pl.BlockSpec(memory_space=pltpu.VMEM),
        scratch_shapes=[
            pltpu.SemaphoreType.DMA,
            pltpu.SemaphoreType.DMA((4, groups)),
            pltpu.SemaphoreType.DMA((4, groups)),
        ],
        compiler_params=pltpu.CompilerParams(
            collective_id=0, has_side_effects=True, vmem_limit_bytes=40 * 2**20
        ),
    )(rows)


def add(a, b):
    return a.astype(jnp.float32) + b.astype(jnp.float32)


def give_back_kernel(part_ref, out_ref, core_in, core_sum, side_in, total, send_sem, recv_sem):
    groups = part_ref.shape[0]
    sp, core, group, side = places()
    across, beside = (group * 2 + 1 - side, core), (sp, 1 - core)
    greet(groups, sp, core, group, side)
    order = list(range(1, groups)) + [0]
    cores, sides, finals = {}, {}, {}
    for kind, which in ((0, 1 - side), (1, side)):
        for o in order:
            to = (group + o) % groups
            cores[kind, o] = remote(
                part_ref.at[to, which, 1 - core],
                core_in.at[to, which],
                send_sem.at[kind, o],
                recv_sem.at[kind, o],
                beside,
            )
            cores[kind, o].start()
    for o in order:
        to = (group + o) % groups
        cores[0, o].wait_recv()
        core_sum[to] = add(part_ref[to, 1 - side, core], core_in[to, 1 - side]).astype(core_sum.dtype)
        sides[o] = remote(
            core_sum.at[to], side_in.at[to], send_sem.at[2, o], recv_sem.at[2, o], across
        )
        sides[o].start()
    for o in order:
        to = (group + o) % groups
        cores[1, o].wait_recv()
        sides[o].wait_recv()
        kept = add(part_ref[to, side, core], core_in[to, side])
        summed = (kept + side_in[to].astype(jnp.float32)).astype(total.dtype)
        if o == 0:
            out_ref[to] = summed
        else:
            total[to] = summed
            finals[o] = remote(
                total.at[to],
                out_ref.at[group],
                send_sem.at[3, o],
                recv_sem.at[3, o],
                (to * 2 + side, core),
            )
            finals[o].start()
    for o in order:
        if o > 0:
            finals[o].wait()
        sides[o].wait_send()
        cores[0, o].wait_send()
        cores[1, o].wait_send()


def give_back(parts):
    groups, _, _, capacity, width = parts.shape
    block = (groups, capacity, width)
    return pl.pallas_call(
        give_back_kernel,
        out_shape=jax.ShapeDtypeStruct(block, parts.dtype),
        in_specs=[pl.BlockSpec(memory_space=pltpu.VMEM)],
        out_specs=pl.BlockSpec(memory_space=pltpu.VMEM),
        scratch_shapes=[
            pltpu.VMEM((groups, 2, capacity, width), parts.dtype),
            pltpu.VMEM(block, parts.dtype),
            pltpu.VMEM(block, parts.dtype),
            pltpu.VMEM(block, parts.dtype),
            pltpu.SemaphoreType.DMA((4, groups)),
            pltpu.SemaphoreType.DMA((4, groups)),
        ],
        compiler_params=pltpu.CompilerParams(
            collective_id=1, has_side_effects=True, vmem_limit_bytes=40 * 2**20
        ),
    )(parts)


def local(
    stream_in,
    query_rows,
    key_rows,
    value_rows,
    removal_key,
    learn_pre,
    log_rate,
    norm_gain,
    out_weight,
    ffn_gain,
    routes,
    route_weight,
    expert_gate,
    expert_up,
    expert_down,
):
    local_read, carry_read, pairs = mix_here(
        query_rows, key_rows, value_rows, removal_key, learn_pre, log_rate
    )
    states = entering_state(pairs, "sp")
    normed = finish(local_read, carry_read, states, norm_gain)
    gathered = lax.all_to_all(normed, "tp", split_axis=0, concat_axis=1, tiled=True)
    attended = stream_in.astype(jnp.float32) + jnp.dot(
        gathered, out_weight, preferred_element_type=jnp.float32
    )
    scaling = lax.rsqrt(jnp.mean(attended * attended, axis=-1, keepdims=True) + NORM_EPS)
    ffn_in = (attended * scaling * ffn_gain.astype(jnp.float32)).astype(jnp.bfloat16)
    half_rows = attended.shape[0]
    width = attended.shape[1]
    experts = lax.axis_size("sp") // 2
    peers = lax.axis_size("sp") * lax.axis_size("tp")
    capacity = 2 * TOPK * half_rows // experts
    pairs = half_rows * TOPK
    expert_ids = routes.reshape(pairs)
    one_hot = (expert_ids[:, None] == jnp.arange(experts, dtype=jnp.int32)[None, :]).astype(
        jnp.int32
    )
    slot_index = jnp.sum(jnp.cumsum(one_hot, axis=0) * one_hot, axis=1) - 1
    send_index = expert_ids * capacity + slot_index
    send_map = (
        jnp.arange(experts * capacity, dtype=jnp.int32)[:, None] == send_index[None, :]
    ).astype(jnp.bfloat16)
    send_map = jnp.sum(send_map.reshape(experts * capacity, half_rows, TOPK), axis=2)
    dispatched = jnp.dot(send_map, ffn_in, preferred_element_type=jnp.float32).astype(jnp.bfloat16)
    arrived = dispatch(dispatched.reshape(experts, capacity, width))
    routed = arrived.reshape(peers * capacity, width)
    gate_act = jnp.dot(routed, expert_gate[0], preferred_element_type=jnp.float32)
    up_act = jnp.dot(routed, expert_up[0], preferred_element_type=jnp.float32)
    hidden = (jax.nn.silu(gate_act) * up_act).astype(jnp.bfloat16)
    partial_out = jnp.dot(hidden, expert_down[0], preferred_element_type=jnp.float32).astype(
        jnp.bfloat16
    )
    returned = give_back(partial_out.reshape(arrived.shape)).reshape(experts * capacity, width)
    back_map = (
        send_index[:, None] == jnp.arange(experts * capacity, dtype=jnp.int32)[None, :]
    ).astype(jnp.bfloat16)
    picked = jnp.dot(back_map, returned, preferred_element_type=jnp.float32).reshape(
        half_rows, TOPK, width
    )
    mixture = jnp.sum(picked * route_weight[:, :, None], axis=1)
    return (attended + mixture).astype(jnp.bfloat16)


def solution(mesh):
    placed = (
        P(("sp", "tp"), None),
        P("sp", "tp"),
        P("sp", "tp"),
        P("sp", "tp"),
        P("sp", "tp"),
        P("sp", "tp"),
        P("sp", "tp"),
        P("tp"),
        P(),
        P(),
        P(("sp", "tp"), None),
        P(("sp", "tp"), None),
        P("sp", None, "tp"),
        P("sp", None, "tp"),
        P("sp", "tp", None),
    )
    return jax.shard_map(
        local, mesh=mesh, in_specs=placed, out_specs=P(("sp", "tp"), None), check_vma=False
    )
```
